32 devices in a mesh: sp: 4 (over y, x), tp: 8 (over z, core).
Axes of the slice: x: 2, y: 2, z: 4, core: 2. Of those that a mesh axis runs over, the one named last changes fastest.
Arguments:
- stream: bfloat16 [4096, 1024], P('tp', 'sp'), may hold values from -6 to 6
- value_weight: bfloat16 [2, 2048, 4096], P(None, 'tp', 'sp'), may hold values from -0.09375 to 0.09375
- gate_weight: bfloat16 [2, 2048, 4096], P(None, 'tp', 'sp'), may hold values from -0.09375 to 0.09375
- conv_taps: bfloat16 [2, 2048, 31], P(None, 'tp'), may hold values from -16 to 16
- norm_gain: bfloat16 [2, 2048], P(None, 'tp'), may hold values from 0.099609375 to 1.8984375
- out_weight: bfloat16 [2, 4096, 2048], P(None, 'tp', 'sp'), may hold values from -4 to 4
- out_gain: bfloat16 [2, 4096], P(None, 'tp'), may hold values from 0.099609375 to 1.8984375
Outputs:
- result: bfloat16 [4096, 1024], P('tp', 'sp')
The draws below stay inside these ranges and needn't reach their ends.
All inputs are finite; a program needn't handle non-finite values.
Results may differ from the reference program's by a relative error of at most 0.015.
Values may be sent and summed in bfloat16 or wider, within the bound.
No kernel may reach another device: no remote copies, remote signals or barrier semaphores. Data moves between devices by JAX's collectives and lax.ppermute only.
A program may use at most 64 MiB of HBM per device.

```python
import jax
import jax.numpy as jnp
from jax import lax

D = 4096
W = 2048
KERNEL = 31
LAYERS = 2
SEQ = 1024


def rising_draw(key, shape, fan, axis):
    base = jax.random.normal(key, shape, jnp.float32)
    position = lax.broadcasted_iota(jnp.float32, shape, axis) / shape[axis]
    return base * fan ** (-0.5) * jnp.exp(position * 2.302585)


def draw_conv_taps(key, part):
    return rising_draw(jax.random.fold_in(key, 11), (LAYERS, W, KERNEL), KERNEL, 1).astype(jnp.bfloat16)


def draw_out_weight(key, part):
    return rising_draw(jax.random.fold_in(key, 23), (LAYERS, D, W), W, 1).astype(jnp.bfloat16)


def levels(key, shape, cuts, least, largest):
    loudness, own = 1.0, jax.random.fold_in(key, 6)
    for dim, blocks in cuts:
        steps = jnp.exp(jax.random.uniform(jax.random.fold_in(own, dim), (blocks,), jnp.float32, least / len(cuts), largest / len(cuts)))
        loudness = loudness * jnp.repeat(steps, shape[dim] // blocks).reshape([-1 if axis == dim else 1 for axis in range(len(shape))])
    return loudness


def gaussian(own_key, extent, scale, bound, pieces=(), dtype=jnp.bfloat16):
    gain = levels(own_key, extent, pieces, -0.22, 0.18) if pieces else 1.0
    result = jax.random.normal(own_key, extent, jnp.float32) * scale * gain
    return jnp.minimum(jnp.maximum(result, -bound), bound).astype(dtype)


def setup_inputs(seed: int = 0) -> dict:
    splits = jax.random.split(jax.random.key(seed), 8)
    stream = gaussian(splits[0], (D, SEQ), 1.0, 6.0, ((0, 8), (1, 4)))
    value_weight = gaussian(splits[1], (LAYERS, W, D), D ** -0.5, 0.09375, ((1, 8), (2, 4)))
    gate_weight = gaussian(splits[2], (LAYERS, W, D), D ** -0.5, 0.09375, ((1, 8), (2, 4)))
    conv_taps = draw_conv_taps(jax.random.fold_in(splits[7], 71), 0)
    norm_gain = jnp.clip(1.0 + 0.18 * jax.random.normal(splits[4], (LAYERS, W), jnp.float32), 0.099609375, 1.8984375).astype(jnp.bfloat16)
    out_weight = draw_out_weight(jax.random.fold_in(splits[7], 71), 0)
    out_gain = jnp.clip(1.0 + 0.18 * jax.random.normal(splits[6], (LAYERS, D), jnp.float32), 0.099609375, 1.8984375).astype(jnp.bfloat16)
    return {"stream": stream, "value_weight": value_weight, "gate_weight": gate_weight, "conv_taps": conv_taps, "norm_gain": norm_gain, "out_weight": out_weight, "out_gain": out_gain}


def reference(stream, value_weight, gate_weight, conv_taps, norm_gain, out_weight, out_gain):
    hidden = stream
    reach = KERNEL // 2
    for layer_index in range(LAYERS):
        value_proj = jnp.dot(value_weight[layer_index], hidden, preferred_element_type=jnp.float32)
        gate_proj = jnp.dot(gate_weight[layer_index], hidden, preferred_element_type=jnp.float32)
        gated = (value_proj * jax.nn.sigmoid(gate_proj)).astype(jnp.bfloat16)
        padded = jnp.pad(gated.astype(jnp.float32), ((0, 0), (reach, reach)))
        kernel_taps = conv_taps[layer_index].astype(jnp.float32)
        convolved = jnp.zeros((W, SEQ), jnp.float32)
        for offset in range(KERNEL):
            convolved = convolved + kernel_taps[:, offset:offset + 1] * padded[:, offset:offset + SEQ]
        conv_wide = lax.optimization_barrier(convolved.astype(jnp.bfloat16)).astype(jnp.float32)
        average = lax.optimization_barrier(jnp.sum(conv_wide, axis=0)) / W
        variance = lax.optimization_barrier(jnp.sum(conv_wide * conv_wide, axis=0)) / W - average * average
        channel_gain = norm_gain[layer_index].astype(jnp.float32)[:, None]
        activated = jax.nn.silu((conv_wide - average) * lax.rsqrt(variance + 1e-05) * channel_gain).astype(jnp.bfloat16)
        branch = jnp.dot(out_weight[layer_index], activated, preferred_element_type=jnp.float32)
        branch_wide = lax.optimization_barrier(branch.astype(jnp.bfloat16)).astype(jnp.float32)
        square_mean = lax.optimization_barrier(jnp.sum(branch_wide * branch_wide, axis=0)) / D
        feature_gain = out_gain[layer_index].astype(jnp.float32)[:, None]
        hidden = (hidden.astype(jnp.float32) + branch_wide * lax.rsqrt(square_mean + 1e-06) * feature_gain).astype(jnp.bfloat16)
    return hidden
```

```python
import functools

import jax
import jax.numpy as jnp
from jax import lax
from jax.experimental import pallas as pl
from jax.experimental.pallas import tpu as pltpu
from jax.sharding import PartitionSpec as P

LAYERS = 2
F32, BF16 = jnp.float32, jnp.bfloat16
NT = (((1,), (1,)), ((), ()))
META = 8
VMEM_LIMIT = 56 * 1024 * 1024


def vmem():
    return pl.BlockSpec(memory_space=pltpu.VMEM)


def smem():
    return pl.BlockSpec(memory_space=pltpu.SMEM)


def call(kernel, out, n_in, scratch=(), flops=10**9):
    return pl.pallas_call(
        kernel,
        out_shape=out,
        in_specs=[smem()] + [vmem()] * n_in,
        out_specs=jax.tree.map(lambda _: vmem(), out),
        scratch_shapes=list(scratch),
        compiler_params=pltpu.CompilerParams(vmem_limit_bytes=VMEM_LIMIT),
        cost_estimate=pl.CostEstimate(flops=flops, bytes_accessed=4 * 10**6, transcendentals=0),
    )


def lanes(index, width):
    return pl.ds(pl.multiple_of(index * width, width), width)


def assemble_kernel(n_tp, idx, *refs):
    pieces, x_ref, meta_ref = refs[:n_tp], refs[n_tp], refs[n_tp + 1]
    rows, width = x_ref.shape[0], pieces[0].shape[1]
    for i, piece in enumerate(pieces):
        at = lanes(idx[i], width)
        x_ref[:, at] = piece[:rows, :]
        meta_ref[:, at] = piece[rows:, :]


def gate_conv_kernel(n_tp, n_sp, idx, x_ref, taps_ref, *refs):
    values, gates, out_ref, scr = refs[:n_sp], refs[n_sp : 2 * n_sp], refs[2 * n_sp], refs[2 * n_sp + 1]
    cols = values[0].shape[1]
    value = gate = None
    for m in range(n_sp):
        block = x_ref[:, lanes(idx[n_tp + m], cols)]
        a = lax.dot_general(block, values[m][...], NT, preferred_element_type=F32)
        b = lax.dot_general(block, gates[m][...], NT, preferred_element_type=F32)
        value = a if value is None else value + a
        gate = b if gate is None else gate + b
    rows = x_ref.shape[0]
    out_rows = out_ref.shape[0]
    halo = (rows - out_rows) // 2
    gated = (value * jax.nn.sigmoid(gate)).astype(BF16).astype(F32)
    first = idx[n_tp + n_sp] - (rows - idx[n_tp + n_sp + 2]) // 2
    position = first + lax.broadcasted_iota(jnp.int32, gated.shape, 0)
    inside = (position >= 0) & (position < idx[n_tp + n_sp + 1])
    gated = jnp.where(inside, gated, 0.0)
    channels = gated.shape[1]
    step = min(128, channels)
    for c in range(channels // step):
        scr[c] = gated[:, c * step : (c + 1) * step]
    kernel_size = taps_ref.shape[0]
    base = halo - kernel_size // 2
    chunk = 32
    for c in range(channels // step):
        for r in range(0, out_rows, chunk):
            total = None
            for j in range(kernel_size):
                term = scr[c, pl.ds(r + j + base, chunk), :] * taps_ref[j : j + 1, c * step : (c + 1) * step]
                total = term if total is None else total + term
            out_ref[r : r + chunk, c * step : (c + 1) * step] = total.astype(BF16)


def activate_kernel(n_tp, layer, idx, meta_ref, *refs):
    pieces, out_ref = refs[:n_tp], refs[n_tp]
    rows, width = pieces[0].shape
    feat = meta_ref.shape[1] // n_tp
    total = square = None
    for piece in pieces:
        x = piece[...].astype(F32)
        total = x if total is None else total + x
        square = x * x if square is None else square + x * x
    count = n_tp * width
    average = jnp.sum(total, axis=1, keepdims=True) / count
    variance = jnp.sum(square, axis=1, keepdims=True) / count - average * average
    scale = lax.rsqrt(variance + 1e-05)

    def activated(i):
        gain = meta_ref[:, lanes(idx[i], feat)][0:1, layer * width : (layer + 1) * width].astype(F32)
        v = (pieces[i][...].astype(F32) - average) * scale * gain
        return v / (1.0 + jnp.exp(-v))

    if width % 128 == 0:
        for i in range(n_tp):
            out_ref[:, lanes(idx[i], width)] = activated(i).astype(BF16)
        return
    first = idx[0] % 2 == 0
    for k in range(n_tp // 2):
        own, other = activated(k), activated(k + n_tp // 2)
        pair = jnp.concatenate([jnp.where(first, own, other), jnp.where(first, other, own)], axis=1)
        out_ref[:, lanes(idx[k] // 2, 2 * width)] = pair.astype(BF16)


def branch_kernel(n_tp, n_sp, idx, act_ref, *refs):
    outs, branch_ref = refs[:n_sp], refs[n_sp]
    cols = outs[0].shape[1]
    total = None
    for m in range(n_sp):
        a = lax.dot_general(act_ref[:, lanes(idx[n_tp + m], cols)], outs[m][...], NT, preferred_element_type=F32)
        total = a if total is None else total + a
    branch_ref[...] = total.astype(BF16)


def last_branch_kernel(n_tp, n_sp, idx, act_ref, *refs):
    outs, branch_ref, square_ref = refs[:n_sp], refs[n_sp], refs[n_sp + 1]
    cols = outs[0].shape[1]
    total = None
    for m in range(n_sp):
        a = lax.dot_general(outs[m][...], act_ref[:, lanes(idx[n_tp + m], cols)], NT, preferred_element_type=F32)
        total = a if total is None else total + a
    narrow = total.astype(BF16)
    branch_ref[...] = narrow
    wide = narrow.astype(F32)
    square_ref[...] = jnp.broadcast_to(jnp.sum(wide * wide, axis=0, keepdims=True), square_ref.shape)


def residual_kernel(n_tp, idx, x_ref, meta_ref, *refs):
    pieces, out_ref, own_ref = refs[:n_tp], refs[n_tp], refs[n_tp + 1]
    rows, width = pieces[0].shape
    skip = (x_ref.shape[0] - rows) // 2
    square = None
    for piece in pieces:
        b = piece[...].astype(F32)
        square = b * b if square is None else square + b * b
    factor = lax.rsqrt(jnp.sum(square, axis=1, keepdims=True) / (n_tp * width) + 1e-06)
    for i, piece in enumerate(pieces):
        at = lanes(idx[i], width)
        gain = meta_ref[:, at][1:2].astype(F32)
        h = x_ref[:, at][skip : skip + rows].astype(F32) + piece[...].astype(F32) * factor * gain
        out_ref[:, at] = h.astype(BF16)
        if i == 0:
            own = own_ref.shape[1]
            edge = (rows - own) // 2
            own_ref[...] = h.astype(BF16).astype(F32)[edge : edge + own].T.astype(BF16)


def finish_kernel(n_features, idx, own_ref, branch_ref, gain_ref, *refs):
    squares, out_ref = refs[:-1], refs[-1]
    total = None
    for s in squares:
        total = s[...] if total is None else total + s[...]
    factor = lax.rsqrt(total[0:1] / n_features + 1e-06)
    out_ref[...] = (own_ref[...].astype(F32) + branch_ref[...].astype(F32) * factor * gain_ref[...]).astype(BF16)


def on_device(n_sp, n_tp, stream, value_weight, gate_weight, conv_taps, norm_gain, out_weight, out_gain):
    features, positions = stream.shape
    channels, kernel_size = conv_taps.shape[1:]
    n_z = n_tp // 2
    n_features = features * n_tp
    reach = -(-(kernel_size // 2) // 8) * 8
    z_core = lax.axis_index("tp")
    j = lax.axis_index("sp")
    z, core = z_core // 2, z_core % 2

    def move(x, axis, count, flip):
        return lax.ppermute(x, axis, [(i, i ^ flip) for i in range(count)])

    def after(x, *deps):
        return lax.optimization_barrier((x, *deps))[0]

    def gather_tp(block):
        mine = [block] + [move(block, "tp", n_tp, 2 * k) for k in range(1, n_z)]
        return mine + [move(b, "tp", n_tp, 1) for b in mine]

    def gather_sp(a, b):
        if n_sp != 4:
            return (
                [a] + [move(a, "sp", n_sp, m) for m in range(1, n_sp)],
                [b] + [move(b, "sp", n_sp, m) for m in range(1, n_sp)],
            )
        ay, bx = move(a, "sp", n_sp, 2), move(b, "sp", n_sp, 1)
        b = after(b, ay)
        ax, by = move(a, "sp", n_sp, 1), move(b, "sp", n_sp, 2)
        ad, bd = move(ay, "sp", n_sp, 1), move(bx, "sp", n_sp, 2)
        return [a, ax, ay, ad], [b, bx, by, bd]

    idx = jnp.stack(
        [2 * (z ^ k) + core for k in range(n_z)]
        + [2 * (z ^ k) + (1 - core) for k in range(n_z)]
        + [j ^ m for m in range(n_sp)]
        + [j * positions, jnp.int32(n_sp * positions), jnp.int32(positions)]
    ).astype(jnp.int32)

    taps = jnp.transpose(conv_taps, (0, 2, 1)).astype(F32)
    last_gain = out_gain[LAYERS - 1].astype(F32)[:, None]

    own = stream.T
    wide = 2 * reach
    left = lax.ppermute(own[positions - wide :], "sp", [(i, i + 1) for i in range(n_sp - 1)])
    right = lax.ppermute(own[:wide], "sp", [(i + 1, i) for i in range(n_sp - 1)])
    meta = jnp.concatenate(
        [norm_gain.reshape(1, LAYERS * channels), out_gain[0:1], jnp.zeros((META - 2, features), BF16)], axis=0
    )
    block = jnp.concatenate([left, own, right, meta], axis=0)
    pieces = gather_tp(block)
    rows = positions + 2 * wide
    hidden, meta_all = call(
        functools.partial(assemble_kernel, n_tp),
        (
            jax.ShapeDtypeStruct((rows, n_features), BF16),
            jax.ShapeDtypeStruct((META, n_features), BF16),
        ),
        n_tp,
    )(idx, *pieces)

    half = features // 2
    for layer in range(LAYERS):
        last = layer == LAYERS - 1
        values, gates = gather_sp(value_weight[layer], gate_weight[layer])
        uppers, lowers = gather_sp(out_weight[layer][:half], out_weight[layer][half:])
        out_rows = rows - 2 * reach
        conv = call(
            functools.partial(gate_conv_kernel, n_tp, n_sp),
            jax.ShapeDtypeStruct((out_rows, channels), BF16),
            2 + 2 * n_sp,
            [pltpu.VMEM((max(1, channels // 128), rows, min(128, channels)), F32)],
        )(idx, hidden, taps[layer], *values, *gates)
        conv_pieces = gather_tp(conv)
        act = call(
            functools.partial(activate_kernel, n_tp, layer),
            jax.ShapeDtypeStruct((out_rows, channels * n_tp), BF16),
            1 + n_tp,
        )(idx, meta_all, *conv_pieces)
        outs = [jnp.concatenate([u, l], axis=0) for u, l in zip(uppers, lowers)]
        if last:
            branch, square = call(
                functools.partial(last_branch_kernel, n_tp, n_sp),
                (
                    jax.ShapeDtypeStruct((features, positions), BF16),
                    jax.ShapeDtypeStruct((8, positions), F32),
                ),
                1 + n_sp,
            )(idx, act, *outs)
            chip = square + move(square, "tp", n_tp, 1)
            squares = [chip] + [move(chip, "tp", n_tp, 2 * k) for k in range(1, n_z)]
            return call(
                functools.partial(finish_kernel, n_features),
                jax.ShapeDtypeStruct((features, positions), BF16),
                3 + n_z,
            )(idx, own_hidden, branch, last_gain, *squares)
        branch = call(
            functools.partial(branch_kernel, n_tp, n_sp),
            jax.ShapeDtypeStruct((out_rows, features), BF16),
            1 + n_sp,
        )(idx, act, *outs)
        branches = gather_tp(branch)
        hidden, own_hidden = call(
            functools.partial(residual_kernel, n_tp),
            (
                jax.ShapeDtypeStruct((out_rows, n_features), BF16),
                jax.ShapeDtypeStruct((features, positions), BF16),
            ),
            2 + n_tp,
        )(idx, hidden, meta_all, *branches)
        rows = out_rows


def solution(mesh):
    return jax.shard_map(
        functools.partial(on_device, mesh.shape["sp"], mesh.shape["tp"]),
        mesh=mesh,
        in_specs=(
            P("tp", "sp"),
            P(None, "tp", "sp"),
            P(None, "tp", "sp"),
            P(None, "tp", None),
            P(None, "tp"),
            P(None, "tp", "sp"),
            P(None, "tp"),
        ),
        out_specs=P("tp", "sp"),
        check_vma=False,
    )
```

```python
import functools

import jax
import jax.numpy as jnp
from jax import lax
from jax.experimental import pallas as pl
from jax.experimental.pallas import tpu as pltpu
from jax.sharding import PartitionSpec as P


LAYERS = 2
F32, BF16 = jnp.float32, jnp.bfloat16
NT = (((1,), (1,)), ((), ()))
META = 8
VMEM_LIMIT = 14 * 1024 * 1024


def vmem():
    return pl.BlockSpec(memory_space=pltpu.VMEM)


def smem():
    return pl.BlockSpec(memory_space=pltpu.SMEM)


def call(kernel, out, n_in, scratch=(), flops=10**9):
    return pl.pallas_call(
        kernel,
        out_shape=out,
        in_specs=[smem()] + [vmem()] * n_in,
        out_specs=jax.tree.map(lambda _: vmem(), out),
        scratch_shapes=list(scratch),
        compiler_params=pltpu.CompilerParams(vmem_limit_bytes=VMEM_LIMIT),
        cost_estimate=pl.CostEstimate(flops=flops, bytes_accessed=4 * 10**6, transcendentals=0),
    )


def lanes(index, width):
    return pl.ds(pl.multiple_of(index * width, width), width)


def assemble_kernel(n_tp, idx, *refs):
    pieces, x_ref, meta_ref = refs[:n_tp], refs[n_tp], refs[n_tp + 1]
    rows, width = x_ref.shape[0], pieces[0].shape[1]
    for i, piece in enumerate(pieces):
        at = lanes(idx[i], width)
        x_ref[:, at] = piece[:rows, :]
        meta_ref[:, at] = piece[rows:, :]


def gate_conv_kernel(n_tp, n_sp, idx, x_ref, taps_ref, *refs):
    values, gates, out_ref, scr = refs[:n_sp], refs[n_sp : 2 * n_sp], refs[2 * n_sp], refs[2 * n_sp + 1]
    cols = values[0].shape[1]
    value = gate = None
    for m in range(n_sp):
        block = x_ref[:, lanes(idx[n_tp + m], cols)]
        a = lax.dot_general(block, values[m][...], NT, preferred_element_type=F32)
        b = lax.dot_general(block, gates[m][...], NT, preferred_element_type=F32)
        value = a if value is None else value + a
        gate = b if gate is None else gate + b
    rows = x_ref.shape[0]
    out_rows = out_ref.shape[0]
    halo = (rows - out_rows) // 2
    gated = (value * jax.nn.sigmoid(gate)).astype(BF16).astype(F32)
    first = idx[n_tp + n_sp] - (rows - idx[n_tp + n_sp + 2]) // 2
    position = first + lax.broadcasted_iota(jnp.int32, gated.shape, 0)
    inside = (position >= 0) & (position < idx[n_tp + n_sp + 1])
    gated = jnp.where(inside, gated, 0.0)
    channels = gated.shape[1]
    step = min(128, channels)
    for c in range(channels // step):
        scr[c] = gated[:, c * step : (c + 1) * step]
    kernel_size = taps_ref.shape[0]
    base = halo - kernel_size // 2
    chunk = 32
    for c in range(channels // step):
        for r in range(0, out_rows, chunk):
            total = None
            for j in range(kernel_size):
                term = scr[c, pl.ds(r + j + base, chunk), :] * taps_ref[j : j + 1, c * step : (c + 1) * step]
                total = term if total is None else total + term
            out_ref[r : r + chunk, c * step : (c + 1) * step] = total.astype(BF16)


def activate_kernel(n_tp, layer, idx, meta_ref, *refs):
    pieces, out_ref = refs[:n_tp], refs[n_tp]
    _, width = pieces[0].shape
    feat = meta_ref.shape[1] // n_tp
    total = square = None
    for piece in pieces:
        x = piece[...].astype(F32)
        total = x if total is None else total + x
        square = x * x if square is None else square + x * x
    count = n_tp * width
    average = jnp.sum(total, axis=1, keepdims=True) / count
    variance = jnp.sum(square, axis=1, keepdims=True) / count - average * average
    scale = lax.rsqrt(variance + 1e-05)

    def activated(i):
        gain = meta_ref[:, lanes(idx[i], feat)][0:1, layer * width : (layer + 1) * width].astype(F32)
        v = (pieces[i][...].astype(F32) - average) * scale * gain
        return v / (1.0 + jnp.exp(-v))

    if width % 128 == 0:
        for i in range(n_tp):
            out_ref[:, lanes(idx[i], width)] = activated(i).astype(BF16)
        return
    first = idx[0] % 2 == 0
    for k in range(n_tp // 2):
        own, other = activated(k), activated(k + n_tp // 2)
        pair = jnp.concatenate([jnp.where(first, own, other), jnp.where(first, other, own)], axis=1)
        out_ref[:, lanes(idx[k] // 2, 2 * width)] = pair.astype(BF16)


def branch_kernel(n_tp, n_sp, idx, act_ref, *refs):
    branch_ref = refs[2 * n_sp]
    half, cols = refs[0].shape
    for part in range(2):
        total = None
        for m in range(n_sp):
            a = lax.dot_general(
                act_ref[:, lanes(idx[n_tp + m], cols)], refs[part * n_sp + m][...], NT, preferred_element_type=F32
            )
            total = a if total is None else total + a
        branch_ref[:, part * half : (part + 1) * half] = total.astype(BF16)


def last_branch_kernel(n_tp, n_sp, idx, act_ref, *refs):
    branch_ref, square_ref = refs[2 * n_sp], refs[2 * n_sp + 1]
    half, cols = refs[0].shape
    square = None
    for part in range(2):
        total = None
        for m in range(n_sp):
            a = lax.dot_general(
                refs[part * n_sp + m][...], act_ref[:, lanes(idx[n_tp + m], cols)], NT, preferred_element_type=F32
            )
            total = a if total is None else total + a
        narrow = total.astype(BF16)
        branch_ref[part * half : (part + 1) * half, :] = narrow
        wide = narrow.astype(F32)
        wide = jnp.sum(wide * wide, axis=0, keepdims=True)
        square = wide if square is None else square + wide
    square_ref[...] = jnp.broadcast_to(square, square_ref.shape)


def residual_kernel(n_tp, idx, x_ref, meta_ref, *refs):
    pieces, out_ref, own_ref = refs[:n_tp], refs[n_tp], refs[n_tp + 1]
    rows, width = pieces[0].shape
    skip = (x_ref.shape[0] - rows) // 2
    square = None
    for piece in pieces:
        b = piece[...].astype(F32)
        square = b * b if square is None else square + b * b
    factor = lax.rsqrt(jnp.sum(square, axis=1, keepdims=True) / (n_tp * width) + 1e-06)
    for i, piece in enumerate(pieces):
        at = lanes(idx[i], width)
        gain = meta_ref[:, at][1:2].astype(F32)
        h = x_ref[:, at][skip : skip + rows].astype(F32) + piece[...].astype(F32) * factor * gain
        out_ref[:, at] = h.astype(BF16)
        if i == 0:
            own = own_ref.shape[1]
            edge = (rows - own) // 2
            own_ref[...] = h.astype(BF16).astype(F32)[edge : edge + own].T.astype(BF16)


def finish_kernel(n_features, idx, own_ref, branch_ref, gain_ref, *refs):
    squares, out_ref = refs[:-1], refs[-1]
    total = None
    for s in squares:
        total = s[...] if total is None else total + s[...]
    factor = lax.rsqrt(total[0:1] / n_features + 1e-06)
    out_ref[...] = (own_ref[...].astype(F32) + branch_ref[...].astype(F32) * factor * gain_ref[...]).astype(BF16)


def on_device(n_sp, n_tp, stream, value_weight, gate_weight, conv_taps, norm_gain, out_weight, out_gain):
    features, positions = stream.shape
    channels, kernel_size = conv_taps.shape[1:]
    n_z = n_tp // 2
    n_features = features * n_tp
    reach = -(-(kernel_size // 2) // 8) * 8
    z_core = lax.axis_index("tp")
    j = lax.axis_index("sp")
    z, core = z_core // 2, z_core % 2

    def move(x, axis, count, flip):
        return lax.ppermute(x, axis, [(i, i ^ flip) for i in range(count)])

    def gather_tp(block):
        mine = [block] + [move(block, "tp", n_tp, 2 * k) for k in range(1, n_z)]
        return mine + [move(b, "tp", n_tp, 1) for b in mine]

    def stream_move(x, flip):
        return move(x, "sp", n_sp, flip)

    def gather_sp(a, b):
        if n_sp != 4:
            return (
                [a] + [stream_move(a, m) for m in range(1, n_sp)],
                [b] + [stream_move(b, m) for m in range(1, n_sp)],
            )
        ay, bx = stream_move(a, 2), stream_move(b, 1)
        ax, by = stream_move(a, 1), stream_move(b, 2)
        ad, bd = stream_move(ay, 1), stream_move(bx, 2)
        return [a, ax, ay, ad], [b, bx, by, bd]

    idx = jnp.stack(
        [2 * (z ^ k) + core for k in range(n_z)]
        + [2 * (z ^ k) + (1 - core) for k in range(n_z)]
        + [j ^ m for m in range(n_sp)]
        + [j * positions, jnp.int32(n_sp * positions), jnp.int32(positions)]
    ).astype(jnp.int32)

    taps = jnp.transpose(conv_taps, (0, 2, 1)).astype(F32)
    last_gain = out_gain[LAYERS - 1].astype(F32)[:, None]

    own = stream.T
    wide = 2 * reach
    left = lax.ppermute(own[positions - wide :], "sp", [(i, i + 1) for i in range(n_sp - 1)])
    right = lax.ppermute(own[:wide], "sp", [(i + 1, i) for i in range(n_sp - 1)])
    meta = jnp.concatenate(
        [norm_gain.reshape(1, LAYERS * channels), out_gain[0:1], jnp.zeros((META - 2, features), BF16)], axis=0
    )
    block = jnp.concatenate([left, own, right, meta], axis=0)
    pieces = gather_tp(block)
    rows = positions + 2 * wide
    hidden, meta_all = call(
        functools.partial(assemble_kernel, n_tp),
        (
            jax.ShapeDtypeStruct((rows, n_features), BF16),
            jax.ShapeDtypeStruct((META, n_features), BF16),
        ),
        n_tp,
    )(idx, *pieces)

    half = features // 2
    for layer in range(LAYERS):
        last = layer == LAYERS - 1
        values, gates = gather_sp(value_weight[layer], gate_weight[layer])
        uppers, lowers = gather_sp(out_weight[layer][:half], out_weight[layer][half:])
        out_rows = rows - 2 * reach
        conv = call(
            functools.partial(gate_conv_kernel, n_tp, n_sp),
            jax.ShapeDtypeStruct((out_rows, channels), BF16),
            2 + 2 * n_sp,
            [pltpu.VMEM((max(1, channels // 128), rows, min(128, channels)), F32)],
        )(idx, hidden, taps[layer], *values, *gates)
        conv_pieces = gather_tp(conv)
        act = call(
            functools.partial(activate_kernel, n_tp, layer),
            jax.ShapeDtypeStruct((out_rows, channels * n_tp), BF16),
            1 + n_tp,
        )(idx, meta_all, *conv_pieces)
        if last:
            branch, square = call(
                functools.partial(last_branch_kernel, n_tp, n_sp),
                (
                    jax.ShapeDtypeStruct((features, positions), BF16),
                    jax.ShapeDtypeStruct((8, positions), F32),
                ),
                1 + 2 * n_sp,
            )(idx, act, *uppers, *lowers)
            chip = square + move(square, "tp", n_tp, 1)
            squares = [chip] + [move(chip, "tp", n_tp, 2 * k) for k in range(1, n_z)]
            return call(
                functools.partial(finish_kernel, n_features),
                jax.ShapeDtypeStruct((features, positions), BF16),
                3 + n_z,
            )(idx, own_hidden, branch, last_gain, *squares)
        branch = call(
            functools.partial(branch_kernel, n_tp, n_sp),
            jax.ShapeDtypeStruct((out_rows, features), BF16),
            1 + 2 * n_sp,
        )(idx, act, *uppers, *lowers)
        branches = gather_tp(branch)
        hidden, own_hidden = call(
            functools.partial(residual_kernel, n_tp),
            (
                jax.ShapeDtypeStruct((out_rows, n_features), BF16),
                jax.ShapeDtypeStruct((features, positions), BF16),
            ),
            2 + n_tp,
        )(idx, hidden, meta_all, *branches)
        rows = out_rows


def solution(mesh):
    n_sp, n_tp = mesh.shape["sp"], mesh.shape["tp"]

    def whole(*args):
        return on_device(n_sp, n_tp, *args)

    return jax.shard_map(
        whole,
        mesh=mesh,
        in_specs=(
            P("tp", "sp"),
            P(None, "tp", "sp"),
            P(None, "tp", "sp"),
            P(None, "tp", None),
            P(None, "tp"),
            P(None, "tp", "sp"),
            P(None, "tp"),
        ),
        out_specs=P("tp", "sp"),
        check_vma=False,
    )
```
